32 devices in a mesh: fs: 16 (over z, y, core), tp: 2 (over x).
Axes of the slice: x: 2, y: 2, z: 4, core: 2. Of those that a mesh axis runs over, the one named last changes fastest.
Arguments:
- tokens: bfloat16 [4096, 2048], P('fs'), may hold values from -6 to 6
- recurrent_input_gain: bfloat16 [2048], replicated, may hold values from 0.099609375 to 1.8984375
- recurrent_branch_weight: bfloat16 [2048, 1024], P('fs', 'tp'), may hold values from -0.125 to 0.125
- output_gate_weight: bfloat16 [2048, 1024], P('fs', 'tp'), may hold values from -0.125 to 0.125
- filter_taps: bfloat16 [4, 1024], P(None, 'tp'), may hold values from -3 to 3
- retention_gate_blocks: bfloat16 [2, 8, 128, 128], P(None, 'tp'), may hold values from -0.5 to 0.5
- input_gate_blocks: bfloat16 [2, 8, 128, 128], P(None, 'tp'), may hold values from -0.5 to 0.5
- channel_decay_rate: float32 [2, 1024], P(None, 'tp'), may hold values from 0 to 0.008, as said below
- position_log_decay: float32 [2, 4096, 1024], P(None, 'fs', 'tp'), may hold values from -0.7 to 0, as said below
- recurrent_output_weight: bfloat16 [1024, 2048], P('tp', 'fs'), may hold values from -0.1875 to 0.1875
- recurrent_output_gain: bfloat16 [2048], replicated, may hold values from 0.099609375 to 1.8984375
- feedforward_norm_gain: bfloat16 [2048], replicated, may hold values from 0.099609375 to 1.8984375
- feedforward_up_weight: bfloat16 [2048, 8192], P('fs', 'tp'), may hold values from -0.125 to 0.125
- feedforward_down_weight: bfloat16 [8192, 2048], P('tp', 'fs'), may hold values from -0.0625 to 0.0625
- feedforward_output_gain: bfloat16 [2048], replicated, may hold values from 0.099609375 to 1.8984375
Outputs:
- layer_out: bfloat16 [4096, 2048], P('fs')
The draws below stay inside these ranges and needn't reach their ends.
Inputs may be any that keep to these rules, and one draw needn't show every extreme that they name: `channel_decay_rate`: positive rates, one for each channel and direction. `position_log_decay`: zero except at a few positions of each sequence and channel.
All inputs are finite; a program needn't handle non-finite values.
Results may differ from the reference program's by a relative error of at most 0.02.
Values may be sent and summed in bfloat16 or wider, within the bound.
A program may use at most 128 MiB of HBM per device.

```python
import math
import jax
import jax.numpy as jnp
from jax import lax

D = 2048
RECURRENT_WIDTH = 1024
BLOCK_W = 128
FF = 8192
CONV_W = 4
SEQUENCE_TOKENS = 256
BLOCKS = 8
TOKENS = 4096
N_FS = 16


def draw_channel_decay_rate(key, part):
    keys = jax.random.split(jax.random.fold_in(key, 11), 3)
    slow = jnp.exp(jax.random.uniform(keys[0], (2, RECURRENT_WIDTH), jnp.float32, math.log(0.05), math.log(0.4))) / SEQUENCE_TOKENS
    fast = jnp.exp(jax.random.uniform(keys[1], (2, RECURRENT_WIDTH), jnp.float32, math.log(0.0025), math.log(0.008)))
    share = 0.5
    picked = jax.random.uniform(keys[2], (2, RECURRENT_WIDTH), jnp.float32) < share
    return jnp.where(picked, fast, slow).astype(jnp.float32)


def draw_position_log_decay(key, part):
    keys = jax.random.split(jax.random.fold_in(key, 23), 2)
    chance = jnp.minimum(3.0 / SEQUENCE_TOKENS, 0.5)
    placed = jax.random.uniform(keys[0], (2, TOKENS, RECURRENT_WIDTH), jnp.float32) < chance
    depth = jax.random.uniform(keys[1], (2, TOKENS, RECURRENT_WIDTH), jnp.float32, math.log(0.5), math.log(0.8))
    return jnp.where(placed, depth, 0.0).astype(jnp.float32)


def level_of(own_key, shape, pieces, smallest, largest):
    level, own = 1.0, jax.random.fold_in(own_key, 6)
    for axis_at, blocks in pieces:
        heights = jnp.exp(jax.random.uniform(jax.random.fold_in(own, axis_at), (blocks,), jnp.float32, smallest / len(pieces), largest / len(pieces)))
        level = level * jnp.repeat(heights, shape[axis_at] // blocks).reshape([-1 if axis == axis_at else 1 for axis in range(len(shape))])
    return level


def centred(rng, extent, width, limit, cuts=(), held_as=jnp.bfloat16):
    entries = jax.random.normal(rng, extent, jnp.float32) * width
    if len(cuts) > 0:
        entries = level_of(rng, extent, cuts, -0.22, 0.18) * entries
    return jnp.clip(entries, min=-limit, max=limit).astype(held_as)


def setup_inputs(seed: int = 0) -> dict:
    streams_of = jax.random.split(jax.random.key(seed), 16)
    tokens = centred(streams_of[0], (TOKENS, D), 1.0, 6.0, ((0, 16),))
    recurrent_input_gain = jnp.clip(1.0 + 0.18 * jax.random.normal(streams_of[1], (D,), jnp.float32), 0.099609375, 1.8984375).astype(jnp.bfloat16)
    recurrent_branch_weight = centred(streams_of[2], (D, RECURRENT_WIDTH), D ** -0.5, 0.125, ((0, 16), (1, 2)))
    output_gate_weight = centred(streams_of[3], (D, RECURRENT_WIDTH), D ** -0.5, 0.125, ((0, 16), (1, 2)))
    filter_taps = centred(streams_of[4], (CONV_W, RECURRENT_WIDTH), CONV_W ** -0.5, 3.0, ((1, 2),))
    retention_gate_blocks = centred(streams_of[5], (2, BLOCKS, BLOCK_W, BLOCK_W), BLOCK_W ** -0.5, 0.5, ((1, 2),))
    input_gate_blocks = centred(streams_of[6], (2, BLOCKS, BLOCK_W, BLOCK_W), BLOCK_W ** -0.5, 0.5, ((1, 2),))
    channel_decay_rate = draw_channel_decay_rate(jax.random.fold_in(streams_of[15], 71), 0)
    position_log_decay = draw_position_log_decay(jax.random.fold_in(streams_of[15], 71), 0)
    recurrent_output_weight = centred(streams_of[9], (RECURRENT_WIDTH, D), RECURRENT_WIDTH ** -0.5, 0.1875, ((0, 2), (1, 16)))
    recurrent_output_gain = jnp.clip(1.0 + 0.18 * jax.random.normal(streams_of[10], (D,), jnp.float32), 0.099609375, 1.8984375).astype(jnp.bfloat16)
    feedforward_norm_gain = jnp.clip(1.0 + 0.18 * jax.random.normal(streams_of[11], (D,), jnp.float32), 0.099609375, 1.8984375).astype(jnp.bfloat16)
    feedforward_up_weight = centred(streams_of[12], (D, FF), D ** -0.5, 0.125, ((0, 16), (1, 2)))
    feedforward_down_weight = centred(streams_of[13], (FF, D), FF ** -0.5, 0.0625, ((0, 2), (1, 16)))
    feedforward_output_gain = jnp.clip(1.0 + 0.18 * jax.random.normal(streams_of[14], (D,), jnp.float32), 0.099609375, 1.8984375).astype(jnp.bfloat16)
    return dict(tokens=tokens, recurrent_input_gain=recurrent_input_gain, recurrent_branch_weight=recurrent_branch_weight, output_gate_weight=output_gate_weight, filter_taps=filter_taps, retention_gate_blocks=retention_gate_blocks, input_gate_blocks=input_gate_blocks, channel_decay_rate=channel_decay_rate, position_log_decay=position_log_decay, recurrent_output_weight=recurrent_output_weight, recurrent_output_gain=recurrent_output_gain, feedforward_norm_gain=feedforward_norm_gain, feedforward_up_weight=feedforward_up_weight, feedforward_down_weight=feedforward_down_weight, feedforward_output_gain=feedforward_output_gain)


EPS = 1e-06
GATE_STEEPNESS = 8.0

def root_norm(values, gain):
    return values * lax.rsqrt(lax.optimization_barrier(jnp.mean(values * values, axis=-1, keepdims=True)) + EPS) * gain.astype(jnp.float32)

def combine(earlier, later):
    return (earlier[0] * later[0], later[0] * earlier[1] + later[1])

def centred_conv(signal, taps):
    length = signal.shape[0]
    width_taps = taps.shape[0]
    left_pad = width_taps // 2
    padded = jnp.pad(signal.astype(jnp.float32), ((left_pad, width_taps - 1 - left_pad), (0, 0)))
    total = jnp.zeros(signal.shape, jnp.float32)
    for offset in range(width_taps):
        total = total + padded[offset:offset + length] * taps[offset].astype(jnp.float32)
    return total.astype(jnp.bfloat16)

def block_map(signal, matrices):
    block_width = matrices.shape[-1]
    shaped = signal.astype(jnp.float32).reshape(signal.shape[0], matrices.shape[0], block_width)
    mapped = jnp.einsum('tnc,ncd->tnd', shaped, matrices.astype(jnp.float32))
    return mapped.reshape(signal.shape)

def linear_recurrence(convolved_output, retention_matrices, input_gate_matrices, decay_rate_row, decay_extra_block, reversed_scan):
    retention_gate = jax.nn.sigmoid(block_map(convolved_output, retention_matrices))
    admit = jax.nn.sigmoid(block_map(convolved_output, input_gate_matrices))
    logarithm_decay = -GATE_STEEPNESS * retention_gate * decay_rate_row[None, :] + decay_extra_block
    decay = jnp.exp(logarithm_decay)
    drive = jnp.sqrt(-jnp.expm1(2.0 * logarithm_decay)) * (admit * convolved_output.astype(jnp.float32))
    _, state = lax.associative_scan(combine, (decay, drive), reverse=reversed_scan, axis=0)
    return state

def reference(tokens, recurrent_input_gain, recurrent_branch_weight, output_gate_weight, filter_taps, retention_gate_blocks, input_gate_blocks, channel_decay_rate, position_log_decay, recurrent_output_weight, recurrent_output_gain, feedforward_norm_gain, feedforward_up_weight, feedforward_down_weight, feedforward_output_gain):

    def single_sequence(scan_operands):
        token_row_block, decay_extra_rows = scan_operands
        normed = root_norm(token_row_block.astype(jnp.float32), recurrent_input_gain).astype(jnp.bfloat16)
        recur_in = jnp.dot(normed, recurrent_branch_weight, preferred_element_type=jnp.float32).astype(jnp.bfloat16)
        gate_in = lax.optimization_barrier(jnp.dot(normed, output_gate_weight, preferred_element_type=jnp.float32).astype(jnp.bfloat16))
        convolved_output = lax.optimization_barrier(centred_conv(recur_in, filter_taps))
        forward_sweep = linear_recurrence(convolved_output, retention_gate_blocks[0], input_gate_blocks[0], channel_decay_rate[0], decay_extra_rows[0], False)
        backward_sweep = linear_recurrence(convolved_output, retention_gate_blocks[1], input_gate_blocks[1], channel_decay_rate[1], decay_extra_rows[1], True)
        hidden = ((forward_sweep + backward_sweep) * jax.nn.gelu(gate_in.astype(jnp.float32))).astype(jnp.bfloat16)
        mixed = jnp.dot(hidden, recurrent_output_weight, preferred_element_type=jnp.float32)
        stream = lax.optimization_barrier((token_row_block.astype(jnp.float32) + root_norm(mixed, recurrent_output_gain)).astype(jnp.bfloat16))
        normed_ff = root_norm(stream.astype(jnp.float32), feedforward_norm_gain).astype(jnp.bfloat16)
        lifted = jnp.square(jax.nn.relu(jnp.dot(normed_ff, feedforward_up_weight, preferred_element_type=jnp.float32))).astype(jnp.bfloat16)
        lowered = jnp.dot(lifted, feedforward_down_weight, preferred_element_type=jnp.float32)
        return (stream.astype(jnp.float32) + root_norm(lowered, feedforward_output_gain)).astype(jnp.bfloat16)
    stacked_directions = tokens.reshape(N_FS, SEQUENCE_TOKENS, D)
    decay_extras = position_log_decay.reshape(2, N_FS, SEQUENCE_TOKENS, RECURRENT_WIDTH).transpose(1, 0, 2, 3)
    final_result = lax.map(single_sequence, (stacked_directions, decay_extras))
    return final_result.reshape(TOKENS, D)
```

```python
import functools

import jax
import jax.numpy as jnp
from jax import lax
from jax.experimental import pallas as pl
from jax.experimental.pallas import tpu as pltpu
from jax.sharding import PartitionSpec as P

EPS = 1e-06
GATE_STEEPNESS = 8.0


def root_norm(values, gain):
    return (
        values
        * lax.rsqrt(jnp.mean(values * values, axis=-1, keepdims=True) + EPS)
        * gain.astype(jnp.float32)
    )


def combine(earlier, later):
    return (earlier[0] * later[0], later[0] * earlier[1] + later[1])


def centred_conv(signal, taps):
    length = signal.shape[0]
    width_taps = taps.shape[0]
    left_pad = width_taps // 2
    padded = jnp.pad(signal.astype(jnp.float32), ((left_pad, width_taps - 1 - left_pad), (0, 0)))
    total = jnp.zeros(signal.shape, jnp.float32)
    for offset in range(width_taps):
        total = total + padded[offset : offset + length] * taps[offset].astype(jnp.float32)
    return total.astype(jnp.bfloat16)


def block_map(signal, matrices):
    block_width = matrices.shape[-1]
    shaped = signal.reshape(signal.shape[0], matrices.shape[0], block_width)
    mapped = jnp.einsum("tnc,ncd->tnd", shaped, matrices, preferred_element_type=jnp.float32)
    return mapped.reshape(signal.shape)


def linear_recurrence(
    convolved_output,
    retention_matrices,
    input_gate_matrices,
    decay_rate_row,
    decay_extra_block,
    reversed_scan,
):
    retention_gate = jax.nn.sigmoid(block_map(convolved_output, retention_matrices))
    admit = jax.nn.sigmoid(block_map(convolved_output, input_gate_matrices))
    logarithm_decay = -GATE_STEEPNESS * retention_gate * decay_rate_row[None, :] + decay_extra_block
    decay = jnp.exp(logarithm_decay)
    drive = jnp.sqrt(-jnp.expm1(2.0 * logarithm_decay)) * (
        admit * convolved_output.astype(jnp.float32)
    )
    _, state = lax.associative_scan(combine, (decay, drive), reverse=reversed_scan, axis=0)
    return state


def per_device(
    tokens,
    recurrent_input_gain,
    recurrent_branch_weight,
    output_gate_weight,
    filter_taps,
    retention_gate_blocks,
    input_gate_blocks,
    channel_decay_rate,
    position_log_decay,
    recurrent_output_weight,
    recurrent_output_gain,
    feedforward_norm_gain,
    feedforward_up_weight,
    feedforward_down_weight,
    feedforward_output_gain,
):
    normed = root_norm(tokens.astype(jnp.float32), recurrent_input_gain).astype(jnp.bfloat16)
    columns = normed
    recur_sum = jnp.dot(
        columns,
        lax.all_gather(recurrent_branch_weight, "fs", axis=0, tiled=True),
        preferred_element_type=jnp.float32,
    )
    gate_sum = jnp.dot(
        columns,
        lax.all_gather(output_gate_weight, "fs", axis=0, tiled=True),
        preferred_element_type=jnp.float32,
    )
    recur_in = recur_sum.astype(jnp.bfloat16)
    gate_in = lax.optimization_barrier(gate_sum.astype(jnp.bfloat16))
    convolved_output = lax.optimization_barrier(centred_conv(recur_in, filter_taps))
    forward_sweep = linear_recurrence(
        convolved_output,
        retention_gate_blocks[0],
        input_gate_blocks[0],
        channel_decay_rate[0],
        position_log_decay[0],
        False,
    )
    backward_sweep = linear_recurrence(
        convolved_output,
        retention_gate_blocks[1],
        input_gate_blocks[1],
        channel_decay_rate[1],
        position_log_decay[1],
        True,
    )
    hidden = ((forward_sweep + backward_sweep) * jax.nn.gelu(gate_in.astype(jnp.float32))).astype(
        jnp.bfloat16
    )
    mixer_cols = lax.all_gather(recurrent_output_weight, "fs", axis=1, tiled=True)
    partial_value = jnp.dot(hidden, mixer_cols, preferred_element_type=jnp.float32)
    mixed = lax.psum(partial_value.astype(jnp.bfloat16), "tp").astype(jnp.float32)
    stream = lax.optimization_barrier(
        (tokens.astype(jnp.float32) + root_norm(mixed, recurrent_output_gain)).astype(jnp.bfloat16)
    )
    normed_ff = root_norm(stream.astype(jnp.float32), feedforward_norm_gain).astype(jnp.bfloat16)
    columns = normed_ff
    lifted_sum = jnp.dot(
        columns,
        lax.all_gather(feedforward_up_weight, "fs", axis=0, tiled=True),
        preferred_element_type=jnp.float32,
    )
    lifted = jnp.square(jax.nn.relu(lifted_sum)).astype(jnp.bfloat16)
    down_cols = lax.all_gather(feedforward_down_weight, "fs", axis=1, tiled=True)
    lowered_part = jnp.dot(lifted, down_cols, preferred_element_type=jnp.float32)
    lowered = lax.psum(lowered_part.astype(jnp.bfloat16), "tp").astype(jnp.float32)
    return (stream.astype(jnp.float32) + root_norm(lowered, feedforward_output_gain)).astype(
        jnp.bfloat16
    )


MESH = pl.DeviceIdType.MESH
F32 = jnp.float32
BF16 = jnp.bfloat16


def shifted_rows(x, d, rows):
    n = x.shape[0]
    r = pltpu.roll(x, d % n, 0)
    keep = rows >= d if d > 0 else rows < n + d
    return jnp.where(keep, r, 0.0)


def one_minus_exp(u):
    poly = -u * (1.0 + u * (1 / 2) * (1.0 + u * (1 / 3) * (1.0 + u * (1 / 4) * (1.0 + u * (1 / 5)))))
    return jnp.where(u > -0.1, poly, 1.0 - jnp.exp(u))


def norm_rows(v, gain):
    return v * lax.rsqrt(jnp.mean(v * v, axis=-1, keepdims=True) + EPS) * gain


class Gather:
    def __init__(self, buf, axis, sems, width):
        self.buf, self.axis, self.width = buf, axis, width
        self.recv, self.right, self.left, self.core, self.ysend = (sems.at[i] for i in range(5))

    def at(self, slot):
        part = pl.ds(pl.multiple_of(slot * self.width, self.width), self.width)
        return self.buf.at[part, :] if self.axis == 0 else self.buf.at[:, part]

    def copy(self, slot, sems, dev, src=None):
        ref = self.at(slot)
        return pltpu.make_async_remote_copy(
            src_ref=ref if src is None else src,
            dst_ref=ref,
            send_sem=sems.at[slot],
            recv_sem=self.recv.at[slot],
            device_id=dev,
            device_id_type=MESH,
        )


def mega_kernel(
    nz,
    x_ref, rg_in, out_in, up_in, dn_in, taps_ref, ret_ref, adm_ref, rate_ref, pld_ref,
    g_in, g_rec, g_ff, g_out,
    o_ref,
    rg_buf, out_buf, up_buf, dn_buf, xn, rin, hid, part_s, part_r, stream, nff, lifted,
    ys, yr, low, xs, xr,
    rg_sem, out_sem, up_sem, dn_sem, loc_sem, mix_sem, nff_sem, ysem, xsem,
):
    f = lax.axis_index("fs")
    t = lax.axis_index("tp")
    z, y, c = f // 4, (f // 2) % 2, f % 2
    rows_n, d_model = x_ref.shape
    ff_q = up_buf.shape[1]

    def dev(zz, yy, cc, tt=t):
        return ((zz * 2 + yy) * 2 + cc, tt)

    def slot_of(zz, yy, cc):
        return (zz * 2 + yy) * 2 + cc

    to_right, to_left = dev(z + 1, y, c), dev(z - 1, y, c)
    to_y, to_c = dev(z, 1 - y, c), dev(z, y, 1 - c)
    to_x = (f, 1 - t)
    w = rg_in.shape[0]
    RG = Gather(rg_buf, 0, rg_sem, w)
    OUT = Gather(out_buf, 1, out_sem, w)
    UP = Gather(up_buf, 0, up_sem, w)
    DN = Gather(dn_buf, 1, dn_sem, w)
    mine = pl.ds(pl.multiple_of(y * ff_q, ff_q), ff_q)
    theirs = pl.ds(pl.multiple_of((1 - y) * ff_q, ff_q), ff_q)

    locals_ = [
        pltpu.make_async_copy(rg_in, RG.at(f), loc_sem.at[0]),
        pltpu.make_async_copy(out_in, OUT.at(f), loc_sem.at[1]),
        pltpu.make_async_copy(up_in.at[:, mine], UP.at(f), loc_sem.at[2]),
        pltpu.make_async_copy(dn_in.at[mine, :], DN.at(f), loc_sem.at[3]),
    ]
    for cp in locals_:
        cp.start()
    up_y = UP.copy(f, UP.ysend, to_y, src=up_in.at[:, theirs])
    dn_y = DN.copy(f, DN.ysend, to_y, src=dn_in.at[theirs, :])

    def start(G, slot, sems, device, cond=None):
        if cond is None:
            G.copy(slot, sems, device).start()
        else:
            @pl.when(cond)
            def _():
                G.copy(slot, sems, device).start()

    def wait_in(G, slot):
        G.copy(slot, G.core, to_c).wait_recv()

    def own(G, slot):
        start(G, slot, G.right, to_right, z < nz - 1)
        start(G, slot, G.left, to_left, z > 0)
        start(G, slot, G.core, to_c)

    def relay(G, r, sides):
        for yy in sides:
            @pl.when(z - r >= 0)
            def _():
                slot = slot_of(z - r, yy, c)
                wait_in(G, slot)
                start(G, slot, G.right, to_right, z < nz - 1)
                start(G, slot, G.core, to_c)

            @pl.when(z + r < nz)
            def _():
                slot = slot_of(z + r, yy, c)
                wait_in(G, slot)
                start(G, slot, G.left, to_left, z > 0)
                start(G, slot, G.core, to_c)

    def drain(G, sides):
        for oz in range(nz):
            for yy in sides:
                slot = slot_of(oz, yy, c)

                @pl.when((oz <= z) & (z < nz - 1))
                def _():
                    G.copy(slot, G.right, to_right).wait_send()

                @pl.when((oz >= z) & (z > 0))
                def _():
                    G.copy(slot, G.left, to_left).wait_send()

    def drain_core(G):
        for oz in range(nz):
            for yy in range(2):
                G.copy(slot_of(oz, yy, c), G.core, to_c).wait_send()

    locals_[0].wait()
    own(RG, f)
    locals_[1].wait()
    own(OUT, f)
    up_y.start()
    dn_y.start()

    chunk = 32

    def norm_in(i, carry):
        rs = pl.ds(pl.multiple_of(i * chunk, chunk), chunk)
        xn[rs, :] = norm_rows(x_ref[rs, :].astype(F32), g_in[...]).astype(BF16)
        return carry

    lax.fori_loop(0, rows_n // chunk, norm_in, 0)

    for G in (RG, OUT):
        start(G, f, G.ysend, to_y)
    for r in range(1, nz):
        for G in (RG, OUT):
            relay(G, r, [y])
        if r == 1:
            locals_[2].wait()
            locals_[3].wait()
            for G in (UP, DN):
                own(G, f)
        for G in (RG, OUT):
            @pl.when(z - r >= 0)
            def _():
                start(G, slot_of(z - r, y, c), G.ysend, to_y)

            @pl.when(z + r < nz)
            def _():
                start(G, slot_of(z + r, y, c), G.ysend, to_y)
    fp = slot_of(z, 1 - y, c)
    for G in (UP, DN):
        wait_in(G, fp)
        own(G, fp)
    for G in (RG, OUT):
        for oz in range(nz):
            slot = slot_of(oz, 1 - y, c)
            wait_in(G, slot)
            start(G, slot, G.core, to_c)
    for oz in range(nz):
        for yy in range(2):
            wait_in(RG, slot_of(oz, yy, 1 - c))

    tile = 256

    def project(i, carry):
        cs = pl.ds(pl.multiple_of(i * tile, tile), tile)
        rin[:, cs] = jnp.dot(xn[...], rg_buf[:, cs], preferred_element_type=F32).astype(BF16)
        return carry

    lax.fori_loop(0, rg_buf.shape[1] // tile, project, 0)

    bw = ret_ref.shape[-1]
    n_blk = ret_ref.shape[1]
    width = n_blk * bw
    rows = lax.broadcasted_iota(jnp.int32, (rows_n, bw), 0)
    n_taps = taps_ref.shape[0]

    def recur(j, carry):
        cs = pl.ds(pl.multiple_of(j * bw, bw), bw)
        gs = pl.ds(pl.multiple_of(width + j * bw, bw), bw)
        sig = rin[:, cs].astype(F32)
        total = jnp.zeros((rows_n, bw), F32)
        for k in range(n_taps):
            d = n_taps // 2 - k
            s = sig if d == 0 else shifted_rows(sig, d, rows)
            total = total + s * taps_ref[k : k + 1, cs]
        conv = total.astype(BF16)
        conv32 = conv.astype(F32)
        both = jnp.zeros((rows_n, bw), F32)
        for w_dir in range(2):
            ret = jax.nn.sigmoid(jnp.dot(conv, ret_ref[w_dir, j], preferred_element_type=F32))
            adm = jax.nn.sigmoid(jnp.dot(conv, adm_ref[w_dir, j], preferred_element_type=F32))
            log_a = -GATE_STEEPNESS * ret * rate_ref[w_dir : w_dir + 1, cs] + pld_ref[w_dir, :, cs]
            a = jnp.exp(log_a)
            b = jnp.sqrt(one_minus_exp(2.0 * log_a)) * (adm * conv32)
            d = 1
            while d < rows_n:
                sd = d if w_dir == 0 else -d
                b = b + a * shifted_rows(b, sd, rows)
                d *= 2
                if d < rows_n:
                    a = a * shifted_rows(a, sd, rows)
            both = both + b
        hid[:, cs] = (both * jax.nn.gelu(rin[:, gs].astype(F32))).astype(BF16)
        return carry

    lax.fori_loop(0, n_blk, recur, 0)

    relay(UP, 1, [0, 1])
    relay(DN, 1, [0, 1])
    for oz in range(nz):
        for yy in range(2):
            wait_in(OUT, slot_of(oz, yy, 1 - c))

    def mix(i, carry):
        cs = pl.ds(pl.multiple_of(i * tile, tile), tile)
        part_s[:, cs] = jnp.dot(hid[...], out_buf[:, cs], preferred_element_type=F32).astype(BF16)
        return carry

    lax.fori_loop(0, d_model // tile, mix, 0)
    mix_cp = pltpu.make_async_remote_copy(
        src_ref=part_s, dst_ref=part_r, send_sem=mix_sem.at[0], recv_sem=mix_sem.at[1],
        device_id=to_x, device_id_type=MESH)
    mix_cp.start()
    mix_cp.wait_recv()
    my_rows = pl.multiple_of(y * rows_n, rows_n)

    def residual(i, carry):
        rs = pl.ds(pl.multiple_of(i * chunk, chunk), chunk)
        mixed = part_s[rs, :].astype(F32) + part_r[rs, :].astype(F32)
        st = (x_ref[rs, :].astype(F32) + norm_rows(mixed, g_rec[...])).astype(BF16)
        stream[rs, :] = st
        ns = pl.ds(pl.multiple_of(my_rows + i * chunk, chunk), chunk)
        nff[ns, :] = norm_rows(st.astype(F32), g_ff[...]).astype(BF16)
        return carry

    lax.fori_loop(0, rows_n // chunk, residual, 0)
    my_nff = nff.at[pl.ds(my_rows, rows_n), :]
    nff_cp = pltpu.make_async_remote_copy(
        src_ref=my_nff, dst_ref=my_nff, send_sem=nff_sem.at[0], recv_sem=nff_sem.at[1],
        device_id=to_y, device_id_type=MESH)
    nff_cp.start()

    relay(UP, 2, [0, 1])
    relay(UP, 3, [0, 1])
    nff_cp.wait_recv()
    for oz in range(nz):
        for yy in range(2):
            wait_in(UP, slot_of(oz, yy, 1 - c))

    def lift(i, carry):
        cs = pl.ds(pl.multiple_of(i * tile, tile), tile)
        v = jnp.dot(nff[...], up_buf[:, cs], preferred_element_type=F32)
        lifted[:, cs] = jnp.square(jnp.maximum(v, 0.0)).astype(BF16)
        return carry

    piece = d_model // nz
    their_rows = pl.multiple_of((1 - y) * rows_n, rows_n)
    edge = (z == 0) | (z == nz - 1)

    def piece_of(p):
        near = (1, 0, 2, 3)[p]
        base = jnp.where(edge, p, near)
        return jnp.where(z < nz // 2, base, nz - 1 - base)

    def cols_of(p):
        return pl.ds(pl.multiple_of(piece_of(p) * piece, piece), piece)

    def y_copy(p):
        return pltpu.make_async_remote_copy(
            src_ref=ys.at[p], dst_ref=yr.at[p], send_sem=ysem.at[0, p], recv_sem=ysem.at[1, p],
            device_id=to_y, device_id_type=MESH)

    def x_copy(p):
        return pltpu.make_async_remote_copy(
            src_ref=xs.at[p], dst_ref=xr.at[p], send_sem=xsem.at[0, p], recv_sem=xsem.at[1, p],
            device_id=to_x, device_id_type=MESH)

    def lower(p):
        oz = piece_of(p)
        for yy in range(2):
            wait_in(DN, slot_of(oz, yy, 1 - c))
        for s in range(piece // tile):
            cs = pl.ds(pl.multiple_of(oz * piece + s * tile, tile), tile)
            out_s = slice(s * tile, (s + 1) * tile)
            ys[p, :, out_s] = jnp.dot(
                lifted[pl.ds(their_rows, rows_n), :], dn_buf[:, cs], preferred_element_type=F32
            ).astype(BF16)
        y_copy(p).start()
        for s in range(piece // tile):
            cs = pl.ds(pl.multiple_of(oz * piece + s * tile, tile), tile)
            low[p, :, s * tile : (s + 1) * tile] = jnp.dot(
                lifted[pl.ds(my_rows, rows_n), :], dn_buf[:, cs], preferred_element_type=F32
            )

    def pass_on(p):
        y_copy(p).wait_recv()
        xs[p] = (low[p] + yr[p].astype(F32)).astype(BF16)
        x_copy(p).start()

    relay(DN, 2, [0, 1])
    lax.fori_loop(0, ff_q // tile, lift, 0)
    lower(0)
    lower(1)
    pass_on(0)
    pass_on(1)
    lower(2)
    relay(DN, 3, [0, 1])
    lower(3)
    pass_on(2)
    pass_on(3)
    for p in range(nz):
        x_copy(p).wait_recv()

    def finish(i, carry):
        rs = pl.ds(pl.multiple_of(i * chunk, chunk), chunk)
        square = jnp.zeros((chunk, 1), F32)
        for p in range(nz):
            v = xs[p, rs, :].astype(F32) + xr[p, rs, :].astype(F32)
            square = square + jnp.sum(v * v, axis=-1, keepdims=True)
        scale = lax.rsqrt(square / d_model + EPS)
        for p in range(nz):
            cs = cols_of(p)
            v = xs[p, rs, :].astype(F32) + xr[p, rs, :].astype(F32)
            o_ref[rs, cs] = (stream[rs, cs].astype(F32) + v * scale * g_out[:, cs]).astype(BF16)
        return carry

    lax.fori_loop(0, rows_n // chunk, finish, 0)

    mix_cp.wait_send()
    nff_cp.wait_send()
    up_y.wait_send()
    dn_y.wait_send()
    for G in (RG, OUT):
        drain(G, [y])
        drain_core(G)
        for oz in range(nz):
            G.copy(slot_of(oz, y, c), G.ysend, to_y).wait_send()
    for G in (UP, DN):
        drain(G, [0, 1])
        drain_core(G)
    for p in range(nz):
        y_copy(p).wait_send()
        x_copy(p).wait_send()


def per_device_kernel(n_fs, *args):
    (tokens, g_in, w_rec, w_gate, taps, ret, adm, rate, pld, w_out, g_rec, g_ff, w_up, w_dn, g_out) = args
    nz = n_fs // 4
    rows, d = tokens.shape
    w_rg = jnp.concatenate([w_rec, w_gate], axis=1)
    ff_q = w_up.shape[1] // 2
    r_w = w_rec.shape[1]
    vm = pl.BlockSpec(memory_space=pltpu.VMEM)
    hb = pl.BlockSpec(memory_space=pl.ANY)
    dma = pltpu.SemaphoreType.DMA

    def gain(g):
        return g.astype(F32).reshape(1, d)

    return pl.pallas_call(
        functools.partial(mega_kernel, nz),
        out_shape=jax.ShapeDtypeStruct((rows, d), BF16),
        in_specs=[vm, hb, hb, hb, hb] + [vm] * 9,
        out_specs=vm,
        scratch_shapes=[
            pltpu.VMEM((d, 2 * r_w), BF16),
            pltpu.VMEM((r_w, d), BF16),
            pltpu.VMEM((d, ff_q), BF16),
            pltpu.VMEM((ff_q, d), BF16),
            pltpu.VMEM((rows, d), BF16),
            pltpu.VMEM((rows, 2 * r_w), BF16),
            pltpu.VMEM((rows, r_w), BF16),
            pltpu.VMEM((rows, d), BF16),
            pltpu.VMEM((rows, d), BF16),
            pltpu.VMEM((rows, d), BF16),
            pltpu.VMEM((2 * rows, d), BF16),
            pltpu.VMEM((2 * rows, ff_q), BF16),
            pltpu.VMEM((nz, rows, d // nz), BF16),
            pltpu.VMEM((nz, rows, d // nz), BF16),
            pltpu.VMEM((nz, rows, d // nz), F32),
            pltpu.VMEM((nz, rows, d // nz), BF16),
            pltpu.VMEM((nz, rows, d // nz), BF16),
            dma((5, n_fs)),
            dma((5, n_fs)),
            dma((5, n_fs)),
            dma((5, n_fs)),
            dma((4,)),
            dma((2,)),
            dma((2,)),
            dma((2, nz)),
            dma((2, nz)),
        ],
        compiler_params=pltpu.CompilerParams(has_side_effects=True, vmem_limit_bytes=62 * 2**20),
    )(
        tokens, w_rg, w_out, w_up, w_dn, taps.astype(F32), ret, adm, rate, pld,
        gain(g_in), gain(g_rec), gain(g_ff), gain(g_out),
    )


def solution(mesh):
    in_specs = (
        P("fs", None),
        P(),
        P("fs", "tp"),
        P("fs", "tp"),
        P(None, "tp"),
        P(None, "tp", None, None),
        P(None, "tp", None, None),
        P(None, "tp"),
        P(None, "fs", "tp"),
        P("tp", "fs"),
        P(),
        P(),
        P("fs", "tp"),
        P("tp", "fs"),
        P(),
    )
    out_specs = P("fs", None)
    n_fs, n_tp = mesh.shape["fs"], mesh.shape["tp"]
    body = functools.partial(per_device_kernel, n_fs) if (n_fs, n_tp) == (16, 2) else per_device
    return jax.shard_map(
        body, mesh=mesh, in_specs=in_specs, out_specs=out_specs, check_vma=False
    )
```

```python
import functools

import jax
import jax.numpy as jnp
from jax import lax
from jax.experimental import pallas as pl
from jax.experimental.pallas import tpu as pltpu
from jax.sharding import PartitionSpec as P

EPS = 1e-06
GATE_STEEPNESS = 8.0


def root_norm(values, gain):
    return (
        values
        * lax.rsqrt(jnp.mean(values * values, axis=-1, keepdims=True) + EPS)
        * gain.astype(jnp.float32)
    )


def combine(earlier, later):
    return (earlier[0] * later[0], later[0] * earlier[1] + later[1])


def centred_conv(signal, taps):
    length = signal.shape[0]
    width_taps = taps.shape[0]
    left_pad = width_taps // 2
    padded = jnp.pad(signal.astype(jnp.float32), ((left_pad, width_taps - 1 - left_pad), (0, 0)))
    total = jnp.zeros(signal.shape, jnp.float32)
    for offset in range(width_taps):
        total = total + padded[offset : offset + length] * taps[offset].astype(jnp.float32)
    return total.astype(jnp.bfloat16)


def block_map(signal, matrices):
    block_width = matrices.shape[-1]
    shaped = signal.reshape(signal.shape[0], matrices.shape[0], block_width)
    mapped = jnp.einsum("tnc,ncd->tnd", shaped, matrices, preferred_element_type=jnp.float32)
    return mapped.reshape(signal.shape)


def linear_recurrence(
    convolved_output,
    retention_matrices,
    input_gate_matrices,
    decay_rate_row,
    decay_extra_block,
    reversed_scan,
):
    retention_gate = jax.nn.sigmoid(block_map(convolved_output, retention_matrices))
    admit = jax.nn.sigmoid(block_map(convolved_output, input_gate_matrices))
    logarithm_decay = -GATE_STEEPNESS * retention_gate * decay_rate_row[None, :] + decay_extra_block
    decay = jnp.exp(logarithm_decay)
    drive = jnp.sqrt(-jnp.expm1(2.0 * logarithm_decay)) * (
        admit * convolved_output.astype(jnp.float32)
    )
    _, state = lax.associative_scan(combine, (decay, drive), reverse=reversed_scan, axis=0)
    return state


def per_device(
    tokens,
    recurrent_input_gain,
    recurrent_branch_weight,
    output_gate_weight,
    filter_taps,
    retention_gate_blocks,
    input_gate_blocks,
    channel_decay_rate,
    position_log_decay,
    recurrent_output_weight,
    recurrent_output_gain,
    feedforward_norm_gain,
    feedforward_up_weight,
    feedforward_down_weight,
    feedforward_output_gain,
):
    normed = root_norm(tokens.astype(jnp.float32), recurrent_input_gain).astype(jnp.bfloat16)
    columns = normed
    recur_sum = jnp.dot(
        columns,
        lax.all_gather(recurrent_branch_weight, "fs", axis=0, tiled=True),
        preferred_element_type=jnp.float32,
    )
    gate_sum = jnp.dot(
        columns,
        lax.all_gather(output_gate_weight, "fs", axis=0, tiled=True),
        preferred_element_type=jnp.float32,
    )
    recur_in = recur_sum.astype(jnp.bfloat16)
    gate_in = lax.optimization_barrier(gate_sum.astype(jnp.bfloat16))
    convolved_output = lax.optimization_barrier(centred_conv(recur_in, filter_taps))
    forward_sweep = linear_recurrence(
        convolved_output,
        retention_gate_blocks[0],
        input_gate_blocks[0],
        channel_decay_rate[0],
        position_log_decay[0],
        False,
    )
    backward_sweep = linear_recurrence(
        convolved_output,
        retention_gate_blocks[1],
        input_gate_blocks[1],
        channel_decay_rate[1],
        position_log_decay[1],
        True,
    )
    hidden = ((forward_sweep + backward_sweep) * jax.nn.gelu(gate_in.astype(jnp.float32))).astype(
        jnp.bfloat16
    )
    mixer_cols = lax.all_gather(recurrent_output_weight, "fs", axis=1, tiled=True)
    partial_value = jnp.dot(hidden, mixer_cols, preferred_element_type=jnp.float32)
    mixed = lax.psum(partial_value.astype(jnp.bfloat16), "tp").astype(jnp.float32)
    stream = lax.optimization_barrier(
        (tokens.astype(jnp.float32) + root_norm(mixed, recurrent_output_gain)).astype(jnp.bfloat16)
    )
    normed_ff = root_norm(stream.astype(jnp.float32), feedforward_norm_gain).astype(jnp.bfloat16)
    columns = normed_ff
    lifted_sum = jnp.dot(
        columns,
        lax.all_gather(feedforward_up_weight, "fs", axis=0, tiled=True),
        preferred_element_type=jnp.float32,
    )
    lifted = jnp.square(jax.nn.relu(lifted_sum)).astype(jnp.bfloat16)
    down_cols = lax.all_gather(feedforward_down_weight, "fs", axis=1, tiled=True)
    lowered_part = jnp.dot(lifted, down_cols, preferred_element_type=jnp.float32)
    lowered = lax.psum(lowered_part.astype(jnp.bfloat16), "tp").astype(jnp.float32)
    return (stream.astype(jnp.float32) + root_norm(lowered, feedforward_output_gain)).astype(
        jnp.bfloat16
    )


MESH = pl.DeviceIdType.MESH
F32 = jnp.float32
BF16 = jnp.bfloat16


def shifted_rows(x, d, rows):
    n = x.shape[0]
    r = pltpu.roll(x, d % n, 0)
    keep = rows >= d if d > 0 else rows < n + d
    return jnp.where(keep, r, 0.0)


def one_minus_exp(u):
    poly = -u * (1.0 + u * (1 / 2) * (1.0 + u * (1 / 3) * (1.0 + u * (1 / 4) * (1.0 + u * (1 / 5)))))
    return jnp.where(u > -0.1, poly, 1.0 - jnp.exp(u))


def norm_rows(v, gain):
    return v * lax.rsqrt(jnp.mean(v * v, axis=-1, keepdims=True) + EPS) * gain


class Gather:
    def __init__(self, buf, axis, sems, width):
        self.buf, self.axis, self.width = buf, axis, width
        self.recv, self.right, self.left, self.core, self.ysend = (sems.at[i] for i in range(5))

    def at(self, slot):
        part = pl.ds(pl.multiple_of(slot * self.width, self.width), self.width)
        return self.buf.at[part, :] if self.axis == 0 else self.buf.at[:, part]

    def copy(self, slot, sems, dev, src=None):
        ref = self.at(slot)
        return pltpu.make_async_remote_copy(
            src_ref=ref if src is None else src,
            dst_ref=ref,
            send_sem=sems.at[slot],
            recv_sem=self.recv.at[slot],
            device_id=dev,
            device_id_type=MESH,
        )


def mega_kernel(
    nz,
    x_ref, rec_in, gate_in, out_in, up_in, dn_in, taps_ref, ret_ref, adm_ref, rate_ref, pld_ref,
    gains,
    o_ref,
    rg_buf, out_buf, up_buf, dn_buf, xn, rin, hid, part_s, part_r, stream, nff, lifted,
    ys, yr, low, xs, xr,
    rg_sem, out_sem, up_sem, dn_sem, loc_sem, mix_sem, nff_sem, ysem, xsem,
):
    f = lax.axis_index("fs")
    t = lax.axis_index("tp")
    z, y, c = f // 4, (f // 2) % 2, f % 2
    rows_n, d_model = x_ref.shape
    ff_q = up_buf.shape[1]

    def dev(zz, yy, cc, tt=t):
        return ((zz * 2 + yy) * 2 + cc, tt)

    def slot_of(zz, yy, cc):
        return (zz * 2 + yy) * 2 + cc

    to_right, to_left = dev(z + 1, y, c), dev(z - 1, y, c)
    to_y, to_c = dev(z, 1 - y, c), dev(z, y, 1 - c)
    to_x = (f, 1 - t)
    w = rec_in.shape[0]
    g_in, g_rec, g_ff, g_out = (gains.at[i : i + 1, :] for i in range(4))
    half = rec_in.shape[1]
    RG = Gather(rg_buf, 0, rg_sem, w)
    OUT = Gather(out_buf, 1, out_sem, w)
    UP = Gather(up_buf, 0, up_sem, w)
    DN = Gather(dn_buf, 1, dn_sem, w)
    mine = pl.ds(pl.multiple_of(y * ff_q, ff_q), ff_q)
    theirs = pl.ds(pl.multiple_of((1 - y) * ff_q, ff_q), ff_q)

    locals_ = [
        pltpu.make_async_copy(rec_in, RG.at(f).at[:, :half], loc_sem.at[0]),
        pltpu.make_async_copy(out_in, OUT.at(f), loc_sem.at[1]),
        pltpu.make_async_copy(up_in.at[:, mine], UP.at(f), loc_sem.at[2]),
        pltpu.make_async_copy(dn_in.at[mine, :], DN.at(f), loc_sem.at[3]),
        pltpu.make_async_copy(gate_in, RG.at(f).at[:, half:], loc_sem.at[4]),
    ]
    for cp in locals_:
        cp.start()
    up_y = UP.copy(f, UP.ysend, to_y, src=up_in.at[:, theirs])
    dn_y = DN.copy(f, DN.ysend, to_y, src=dn_in.at[theirs, :])

    def start(G, slot, sems, device, cond=None):
        if cond is None:
            G.copy(slot, sems, device).start()
        else:
            @pl.when(cond)
            def _():
                G.copy(slot, sems, device).start()

    def wait_in(G, slot):
        G.copy(slot, G.core, to_c).wait_recv()

    def own(G, slot):
        start(G, slot, G.right, to_right, z < nz - 1)
        start(G, slot, G.left, to_left, z > 0)
        start(G, slot, G.core, to_c)

    def relay(G, r, sides):
        for yy in sides:
            @pl.when(z - r >= 0)
            def _():
                slot = slot_of(z - r, yy, c)
                wait_in(G, slot)
                start(G, slot, G.right, to_right, z < nz - 1)
                start(G, slot, G.core, to_c)

            @pl.when(z + r < nz)
            def _():
                slot = slot_of(z + r, yy, c)
                wait_in(G, slot)
                start(G, slot, G.left, to_left, z > 0)
                start(G, slot, G.core, to_c)

    def drain(G, sides):
        for oz in range(nz):
            for yy in sides:
                slot = slot_of(oz, yy, c)

                @pl.when((oz <= z) & (z < nz - 1))
                def _():
                    G.copy(slot, G.right, to_right).wait_send()

                @pl.when((oz >= z) & (z > 0))
                def _():
                    G.copy(slot, G.left, to_left).wait_send()

    def drain_core(G):
        for oz in range(nz):
            for yy in range(2):
                G.copy(slot_of(oz, yy, c), G.core, to_c).wait_send()

    locals_[0].wait()
    locals_[4].wait()
    own(RG, f)
    locals_[1].wait()
    own(OUT, f)
    up_y.start()
    dn_y.start()

    chunk = 32

    def norm_in(i, carry):
        rs = pl.ds(pl.multiple_of(i * chunk, chunk), chunk)
        xn[rs, :] = norm_rows(x_ref[rs, :].astype(F32), g_in[...]).astype(BF16)
        return carry

    lax.fori_loop(0, rows_n // chunk, norm_in, 0)

    for G in (RG, OUT):
        start(G, f, G.ysend, to_y)
    for r in range(1, nz):
        for G in (RG, OUT):
            relay(G, r, [y])
        if r == 1:
            locals_[2].wait()
            own(UP, f)
        if r == 2:
            locals_[3].wait()
            own(DN, f)
        for G in (RG, OUT):
            @pl.when(z - r >= 0)
            def _():
                start(G, slot_of(z - r, y, c), G.ysend, to_y)

            @pl.when(z + r < nz)
            def _():
                start(G, slot_of(z + r, y, c), G.ysend, to_y)
    fp = slot_of(z, 1 - y, c)
    for G in (UP, DN):
        wait_in(G, fp)
        own(G, fp)
    for G in (RG, OUT):
        for oz in range(nz):
            slot = slot_of(oz, 1 - y, c)
            wait_in(G, slot)
            start(G, slot, G.core, to_c)
    for oz in range(nz):
        for yy in range(2):
            wait_in(RG, slot_of(oz, yy, 1 - c))

    tile = 256

    def project(i, carry):
        cs = pl.ds(pl.multiple_of(i * tile, tile), tile)
        rin[:, cs] = jnp.dot(xn[...], rg_buf[:, cs], preferred_element_type=F32).astype(BF16)
        return carry

    lax.fori_loop(0, rg_buf.shape[1] // tile, project, 0)

    bw = ret_ref.shape[-1]
    n_blk = ret_ref.shape[1]
    width = n_blk * bw
    rows = lax.broadcasted_iota(jnp.int32, (rows_n, bw), 0)
    n_taps = taps_ref.shape[0]

    def recur(j, carry):
        cs = pl.ds(pl.multiple_of(j * bw, bw), bw)
        gs = pl.ds(pl.multiple_of(width + j * bw, bw), bw)
        sig = rin[:, cs].astype(F32)
        total = jnp.zeros((rows_n, bw), F32)
        for k in range(n_taps):
            d = n_taps // 2 - k
            s = sig if d == 0 else shifted_rows(sig, d, rows)
            total = total + s * taps_ref[k : k + 1, cs]
        conv = total.astype(BF16)
        conv32 = conv.astype(F32)
        both = jnp.zeros((rows_n, bw), F32)
        for w_dir in range(2):
            ret = jax.nn.sigmoid(jnp.dot(conv, ret_ref[w_dir, j], preferred_element_type=F32))
            adm = jax.nn.sigmoid(jnp.dot(conv, adm_ref[w_dir, j], preferred_element_type=F32))
            log_a = -GATE_STEEPNESS * ret * rate_ref[w_dir : w_dir + 1, cs] + pld_ref[w_dir, :, cs]
            a = jnp.exp(log_a)
            b = jnp.sqrt(one_minus_exp(2.0 * log_a)) * (adm * conv32)
            d = 1
            while d < rows_n:
                sd = d if w_dir == 0 else -d
                b = b + a * shifted_rows(b, sd, rows)
                d *= 2
                if d < rows_n:
                    a = a * shifted_rows(a, sd, rows)
            both = both + b
        hid[:, cs] = (both * jax.nn.gelu(rin[:, gs].astype(F32))).astype(BF16)
        return carry

    relay(UP, 1, [y])
    relay(DN, 1, [y])
    lax.fori_loop(0, n_blk, recur, 0)
    relay(UP, 1, [1 - y])
    relay(DN, 1, [1 - y])
    for oz in range(nz):
        for yy in range(2):
            wait_in(OUT, slot_of(oz, yy, 1 - c))

    def mix(i, carry):
        cs = pl.ds(pl.multiple_of(i * tile, tile), tile)
        part_s[:, cs] = jnp.dot(hid[...], out_buf[:, cs], preferred_element_type=F32).astype(BF16)
        return carry

    lax.fori_loop(0, d_model // tile, mix, 0)
    mix_cp = pltpu.make_async_remote_copy(
        src_ref=part_s, dst_ref=part_r, send_sem=mix_sem.at[0], recv_sem=mix_sem.at[1],
        device_id=to_x, device_id_type=MESH)
    mix_cp.start()
    relay(UP, 2, [y])
    relay(DN, 2, [y])
    mix_cp.wait_recv()
    my_rows = pl.multiple_of(y * rows_n, rows_n)

    def residual(i, carry):
        rs = pl.ds(pl.multiple_of(i * chunk, chunk), chunk)
        mixed = part_s[rs, :].astype(F32) + part_r[rs, :].astype(F32)
        st = (x_ref[rs, :].astype(F32) + norm_rows(mixed, g_rec[...])).astype(BF16)
        stream[rs, :] = st
        ns = pl.ds(pl.multiple_of(my_rows + i * chunk, chunk), chunk)
        nff[ns, :] = norm_rows(st.astype(F32), g_ff[...]).astype(BF16)
        return carry

    lax.fori_loop(0, rows_n // chunk, residual, 0)
    my_nff = nff.at[pl.ds(my_rows, rows_n), :]
    nff_cp = pltpu.make_async_remote_copy(
        src_ref=my_nff, dst_ref=my_nff, send_sem=nff_sem.at[0], recv_sem=nff_sem.at[1],
        device_id=to_y, device_id_type=MESH)
    nff_cp.start()

    relay(UP, 2, [1 - y])
    relay(DN, 2, [1 - y])
    relay(UP, 3, [y, 1 - y])
    nff_cp.wait_recv()
    for oz in range(nz):
        for yy in range(2):
            wait_in(UP, slot_of(oz, yy, 1 - c))

    def lift(i, carry):
        cs = pl.ds(pl.multiple_of(i * tile, tile), tile)
        v = jnp.dot(nff[...], up_buf[:, cs], preferred_element_type=F32)
        lifted[:, cs] = jnp.square(jnp.maximum(v, 0.0)).astype(BF16)
        return carry

    piece = d_model // nz
    their_rows = pl.multiple_of((1 - y) * rows_n, rows_n)
    edge = (z == 0) | (z == nz - 1)

    def piece_of(p):
        near = (1, 0, 2, 3)[p]
        base = jnp.where(edge, p, near)
        return jnp.where(z < nz // 2, base, nz - 1 - base)

    per = piece // tile

    def cols_of(q):
        start_at = piece_of(q // per) * piece + (q % per) * tile
        return pl.ds(pl.multiple_of(start_at, tile), tile)

    def y_copy(p):
        return pltpu.make_async_remote_copy(
            src_ref=ys.at[p], dst_ref=yr.at[p], send_sem=ysem.at[0, p], recv_sem=ysem.at[1, p],
            device_id=to_y, device_id_type=MESH)

    def x_copy(p):
        return pltpu.make_async_remote_copy(
            src_ref=xs.at[p], dst_ref=xr.at[p], send_sem=xsem.at[0, p], recv_sem=xsem.at[1, p],
            device_id=to_x, device_id_type=MESH)

    def lower(p):
        oz = piece_of(p)
        for yy in range(2):
            wait_in(DN, slot_of(oz, yy, 1 - c))
        for q in range(p * per, (p + 1) * per):
            ys[q] = jnp.dot(
                lifted[pl.ds(their_rows, rows_n), :],
                dn_buf[:, cols_of(q)],
                preferred_element_type=F32,
            ).astype(BF16)
            y_copy(q).start()
        for q in range(p * per, (p + 1) * per):
            low[q] = jnp.dot(
                lifted[pl.ds(my_rows, rows_n), :],
                dn_buf[:, cols_of(q)],
                preferred_element_type=F32,
            )

    def pass_on(p):
        y_copy(p).wait_recv()
        xs[p] = (low[p] + yr[p].astype(F32)).astype(BF16)
        x_copy(p).start()

    lax.fori_loop(0, ff_q // tile, lift, 0)
    lower(0)
    lower(1)
    for q in range(2 * per):
        pass_on(q)
    lower(2)
    for q in range(2 * per, 3 * per):
        pass_on(q)
    relay(DN, 3, [y, 1 - y])
    lower(3)
    for q in range(3 * per, 4 * per):
        pass_on(q)
    for q in range(nz * per):
        x_copy(q).wait_recv()

    def finish(i, carry):
        rs = pl.ds(pl.multiple_of(i * chunk, chunk), chunk)
        square = jnp.zeros((chunk, 1), F32)
        for p in range(nz * per):
            v = xs[p, rs, :].astype(F32) + xr[p, rs, :].astype(F32)
            square = square + jnp.sum(v * v, axis=-1, keepdims=True)
        scale = lax.rsqrt(square / d_model + EPS)
        for p in range(nz * per):
            cs = cols_of(p)
            v = xs[p, rs, :].astype(F32) + xr[p, rs, :].astype(F32)
            o_ref[rs, cs] = (stream[rs, cs].astype(F32) + v * scale * g_out[:, cs]).astype(BF16)
        return carry

    lax.fori_loop(0, rows_n // chunk, finish, 0)

    mix_cp.wait_send()
    nff_cp.wait_send()
    up_y.wait_send()
    dn_y.wait_send()
    for G in (RG, OUT):
        drain(G, [y])
        drain_core(G)
        for oz in range(nz):
            G.copy(slot_of(oz, y, c), G.ysend, to_y).wait_send()
    for G in (UP, DN):
        drain(G, [0, 1])
        drain_core(G)
    for p in range(nz * per):
        y_copy(p).wait_send()
        x_copy(p).wait_send()


def per_device_kernel(n_fs, *args):
    (tokens, g_in, w_rec, w_gate, taps, ret, adm, rate, pld, w_out, g_rec, g_ff, w_up, w_dn, g_out) = args
    nz = n_fs // 4
    rows, d = tokens.shape
    tile = 256
    np_ = d // tile
    gains = jnp.stack([g_in, g_rec, g_ff, g_out]).astype(F32)
    ff_q = w_up.shape[1] // 2
    r_w = w_rec.shape[1]
    vm = pl.BlockSpec(memory_space=pltpu.VMEM)
    hb = pl.BlockSpec(memory_space=pl.ANY)
    dma = pltpu.SemaphoreType.DMA

    return pl.pallas_call(
        functools.partial(mega_kernel, nz),
        out_shape=jax.ShapeDtypeStruct((rows, d), BF16),
        in_specs=[vm, hb, hb, hb, hb, hb] + [vm] * 6,
        out_specs=vm,
        scratch_shapes=[
            pltpu.VMEM((d, 2 * r_w), BF16),
            pltpu.VMEM((r_w, d), BF16),
            pltpu.VMEM((d, ff_q), BF16),
            pltpu.VMEM((ff_q, d), BF16),
            pltpu.VMEM((rows, d), BF16),
            pltpu.VMEM((rows, 2 * r_w), BF16),
            pltpu.VMEM((rows, r_w), BF16),
            pltpu.VMEM((rows, d), BF16),
            pltpu.VMEM((rows, d), BF16),
            pltpu.VMEM((rows, d), BF16),
            pltpu.VMEM((2 * rows, d), BF16),
            pltpu.VMEM((2 * rows, ff_q), BF16),
            pltpu.VMEM((np_, rows, tile), BF16),
            pltpu.VMEM((np_, rows, tile), BF16),
            pltpu.VMEM((np_, rows, tile), F32),
            pltpu.VMEM((np_, rows, tile), BF16),
            pltpu.VMEM((np_, rows, tile), BF16),
            dma((5, n_fs)),
            dma((5, n_fs)),
            dma((5, n_fs)),
            dma((5, n_fs)),
            dma((5,)),
            dma((2,)),
            dma((2,)),
            dma((2, np_)),
            dma((2, np_)),
        ],
        compiler_params=pltpu.CompilerParams(has_side_effects=True, vmem_limit_bytes=62 * 2**20),
    )(
        tokens, w_rec, w_gate, w_out, w_up, w_dn, taps.astype(F32), ret, adm, rate, pld, gains,
    )


def solution(mesh):
    in_specs = (
        P("fs", None),
        P(),
        P("fs", "tp"),
        P("fs", "tp"),
        P(None, "tp"),
        P(None, "tp", None, None),
        P(None, "tp", None, None),
        P(None, "tp"),
        P(None, "fs", "tp"),
        P("tp", "fs"),
        P(),
        P(),
        P("fs", "tp"),
        P("tp", "fs"),
        P(),
    )
    out_specs = P("fs", None)
    n_fs, n_tp = mesh.shape["fs"], mesh.shape["tp"]
    body = functools.partial(per_device_kernel, n_fs) if (n_fs, n_tp) == (16, 2) else per_device
    return jax.shard_map(
        body, mesh=mesh, in_specs=in_specs, out_specs=out_specs, check_vma=False
    )
```
